32 devices in a mesh: fs: 4 (over z), rep: 4 (over y, x), tp: 2 (over core).
Axes of the slice: x: 2, y: 2, z: 4, core: 2. Of those that a mesh axis runs over, the one named last changes fastest.
Arguments:
- inputs: bfloat16 [4096, 2048], P(('fs', 'rep')), may hold values from -6 to 6
- cot_query: bfloat16 [4096, 2048], P(('fs', 'rep'), 'tp'), may hold values from -0.09375 to 0.09375
- cot_key: bfloat16 [4096, 512], P(('fs', 'rep'), 'tp'), may hold values from -0.09375 to 0.09375
- basis_query: bfloat16 [2048, 512], P('fs'), may hold values from -0.125 to 0.125
- basis_key: bfloat16 [2048, 512], P('fs'), may hold values from -0.125 to 0.125
- weight_query: float32 [2048, 2048], P('fs', 'tp'), may hold values from -0.125 to 0.125
- weight_key: float32 [2048, 512], P('fs', 'tp'), may hold values from -0.125 to 0.125
- moments_query: float32 [2, 512, 2048], P(None, 'fs', 'tp'), may hold values from -8 to 8, as said below
- moments_key: float32 [2, 512, 512], P(None, 'fs', 'tp'), may hold values from -8 to 8, as said below
Outputs:
- step_query: float32 [2048, 2048], P('fs', 'tp')
- step_key: float32 [2048, 512], P('fs', 'tp')
- new_weight_query: float32 [2048, 2048], P('fs', 'tp')
- new_weight_key: float32 [2048, 512], P('fs', 'tp')
- copy_query: bfloat16 [2048, 2048], P(None, 'tp')
- copy_key: bfloat16 [2048, 512], P(None, 'tp')
- new_moments_query: float32 [2, 512, 2048], P(None, 'fs', 'tp')
- new_moments_key: float32 [2, 512, 512], P(None, 'fs', 'tp')
The draws below stay inside these ranges and needn't reach their ends.
Inputs may be any that keep to these rules, and one draw needn't show every extreme that they name: `moments_query`: entry 1 along the first dimension is positive. `moments_key`: entry 1 along the first dimension is positive.
All inputs are finite; a program needn't handle non-finite values.
Results may differ from the reference program's by a relative error of at most 0.009.
Values may be sent and summed in bfloat16 or wider, within the bound.
A program may use at most 64 MiB of HBM per device.

```python
import math
import jax
import jax.numpy as jnp
from jax import lax

D = 2048
DQ = 2048
DKV = 512
RANK = 512
TOKENS = 4096


def moment_draw(key, columns):
    first_key, second_key = jax.random.split(jax.random.fold_in(key, 7))
    position = jnp.arange(RANK, dtype=jnp.float32) / max(RANK - 1, 1)
    level = 0.1 * 10.0 ** position[:, None]
    first = jnp.clip(jax.random.normal(first_key, (RANK, columns), jnp.float32), -4.0, 4.0)
    spread = jnp.exp(jax.random.uniform(second_key, (RANK, columns), jnp.float32, math.log(0.05), math.log(0.5)))
    return jnp.stack([first * level, spread * level * level]).astype(jnp.float32)


def draw_moments_query(key, part):
    return moment_draw(key, DQ)


def draw_moments_key(key, part):
    return moment_draw(key, DKV)


def shard_levels(stream_key, shape, shards, smallest, largest):
    gain, own = 1.0, jax.random.fold_in(stream_key, 6)
    for dim, shards_of in shards:
        heights = jnp.exp(jax.random.uniform(jax.random.fold_in(own, dim), (shards_of,), jnp.float32, smallest / len(shards), largest / len(shards)))
        gain = gain * jnp.repeat(heights, shape[dim] // shards_of).reshape([-1 if axis == dim else 1 for axis in range(len(shape))])
    return gain


def scatter_about(own_key, shape, width, limit, cuts=(), kind=jnp.bfloat16):
    gain = shard_levels(own_key, shape, cuts, -0.22, 0.18) if cuts else 1.0
    drawn = jax.random.normal(own_key, shape, jnp.float32) * width * gain
    return jnp.minimum(jnp.maximum(drawn, -limit), limit).astype(kind)


def setup_inputs(seed: int = 0) -> dict:
    streams_of = jax.random.split(jax.random.key(seed), 10)
    inputs = scatter_about(streams_of[0], (TOKENS, D), 1.0, 6.0, ((0, 16),))
    cot_query = scatter_about(streams_of[1], (TOKENS, DQ), (1.0 / (TOKENS ** 0.5)), 0.09375, ((0, 16), (1, 2)))
    cot_key = scatter_about(streams_of[2], (TOKENS, DKV), (1.0 / (TOKENS ** 0.5)), 0.09375, ((0, 16), (1, 2)))
    basis_query = scatter_about(streams_of[3], (D, RANK), D ** -0.5, 0.125, ((0, 4),))
    basis_key = scatter_about(streams_of[4], (D, RANK), D ** -0.5, 0.125, ((0, 4),))
    weight_query = scatter_about(streams_of[5], (D, DQ), D ** -0.5, 0.125, ((0, 4), (1, 2)), jnp.float32)
    weight_key = scatter_about(streams_of[6], (D, DKV), D ** -0.5, 0.125, ((0, 4), (1, 2)), jnp.float32)
    moments_query = draw_moments_query(jax.random.fold_in(streams_of[9], 71), 0)
    moments_key = draw_moments_key(jax.random.fold_in(streams_of[9], 71), 0)
    return dict(inputs=inputs, cot_query=cot_query, cot_key=cot_key, basis_query=basis_query, basis_key=basis_key, weight_query=weight_query, weight_key=weight_key, moments_query=moments_query, moments_key=moments_key)


def reference(inputs, cot_query, cot_key, basis_query, basis_key, weight_query, weight_key, moments_query, moments_key):
    span = math.gcd(TOKENS, 8192)
    blocks = TOKENS // span
    in_blocks = inputs.reshape(blocks, span, D)
    query_blocks = cot_query.reshape(blocks, span, DQ)
    key_blocks = cot_key.reshape(blocks, span, DKV)

    def add_block(totals, pieces):
        rows, c_query, c_key = pieces
        rows = rows.astype(jnp.float32)
        grad_q = jnp.dot(rows.T, c_query.astype(jnp.float32), precision=lax.Precision.HIGHEST, preferred_element_type=jnp.float32)
        grad_k = jnp.dot(rows.T, c_key.astype(jnp.float32), precision=lax.Precision.HIGHEST, preferred_element_type=jnp.float32)
        return ((totals[0] + grad_q, totals[1] + grad_k), None)
    start = (jnp.zeros((D, DQ), jnp.float32), jnp.zeros((D, DKV), jnp.float32))
    (grad_query, grad_key), unused = lax.scan(add_block, start, (in_blocks, query_blocks, key_blocks))

    def update(grad, basis, weight, moments):
        low = jnp.dot(basis.astype(jnp.float32).T, grad, precision=lax.Precision.HIGHEST, preferred_element_type=jnp.float32)
        first = 0.9 * moments[0] + 0.1 * low
        second = 0.95 * moments[1] + 0.05 * low * low
        normed = first / (jnp.sqrt(second) + 1e-08)
        scale = lax.rsqrt(jnp.mean(normed * normed) + 1e-06)
        direction = normed.astype(jnp.bfloat16)
        step = scale * jnp.dot(basis, direction, preferred_element_type=jnp.float32)
        new_weight = weight - 0.02 * step
        return (step, new_weight, new_weight.astype(jnp.bfloat16), jnp.stack([first, second]))
    step_q, weight_q, copy_q, moments_q = update(grad_query, basis_query, weight_query, moments_query)
    step_k, weight_k, copy_k, moments_k = update(grad_key, basis_key, weight_key, moments_key)
    return (step_q, step_k, weight_q, weight_k, copy_q, copy_k, moments_q, moments_k)
```

```python
import functools
import jax
import jax.numpy as jnp
from jax import lax
from jax.experimental import pallas as pl
from jax.experimental.pallas import tpu as pltpu
from jax.sharding import PartitionSpec as P

MESH = pl.DeviceIdType.MESH
LANES = 128


def each(start, stop, body):
    if stop - start <= 4:
        for i in range(start, stop):
            body(i)
    else:
        lax.fori_loop(start, stop, lambda i, carry: (body(i), carry)[1], 0)


def remote(src, dst, send_sem, recv_sem, **device):
    return pltpu.make_async_remote_copy(
        src_ref=src,
        dst_ref=dst,
        send_sem=send_sem,
        recv_sem=recv_sem,
        device_id=device,
        device_id_type=MESH,
    )


def exchange(
    fs,
    rep,
    inputs,
    cot_query,
    cot_key,
    basis,
    wide_query,
    wide_key,
    moments_query,
    moments_key,
    basis_all,
    weight_query_all,
    weight_key_all,
    dir_query,
    dir_key,
    low_query,
    low_key,
    totals,
    factor,
    part_send,
    part_recv,
    slab,
    slab_recv,
    low_all,
    squares,
    pair,
    az_s,
    az_r,
    ap_s,
    ap_r,
    ez_s,
    ez_r,
    ep_s,
    ep_r,
    bp_s,
    bp_r,
    bz_s,
    bz_r,
    lp_s,
    lp_r,
    dz_s,
    dz_r,
    qz_s,
    qz_r,
    pair_s,
    pair_r,
    local,
):
    f, r, c = lax.axis_index("fs"), lax.axis_index("rep"), lax.axis_index("tp")
    height = basis.shape[1]
    part = height // rep
    rank = basis.shape[2]
    rows = rank // fs
    tokens = inputs.shape[0]
    per = part_send.shape[0] // rep
    query_units = cot_query.shape[1] // LANES
    units = query_units + cot_key.shape[1] // LANES

    def ahead(i):
        return lax.rem(f + i, fs)

    def behind(i):
        return lax.rem(f + fs - i, fs)

    def beside(j):
        return lax.rem(r + j, rep)

    def piece(source, owner):
        return pl.ds(pl.multiple_of(source * height + owner * part, part), part)

    own_part = pl.ds(pl.multiple_of(r * part, part), part)
    own_block = pl.ds(pl.multiple_of(f * height, height), height)

    def low_rows(source):
        return pl.ds(pl.multiple_of(source * rows, rows), rows)

    barrier = pltpu.get_barrier_semaphore()

    def greet_fs(i):
        pl.semaphore_signal(barrier, inc=1, device_id={"fs": ahead(i)}, device_id_type=MESH)

    def greet_rep(j):
        pl.semaphore_signal(barrier, inc=1, device_id={"rep": beside(j)}, device_id_type=MESH)

    each(1, fs, greet_fs)
    each(1, rep, greet_rep)
    pl.semaphore_signal(barrier, inc=1, device_id={"tp": 1 - c}, device_id_type=MESH)
    pl.semaphore_wait(barrier, fs + rep - 1)

    def basis_fs(i, source, target):
        return remote(
            basis.at[c, own_part],
            basis_all.at[c, piece(source, r)],
            az_s.at[target],
            az_r.at[source],
            fs=target,
        )

    each(1, fs, lambda i: basis_fs(i, f, ahead(i)).start())

    weights = ((wide_query, weight_query_all), (wide_key, weight_key_all))

    def weight_fs(x, source, target):
        return remote(
            weights[x][0].at[own_part],
            weights[x][1].at[piece(source, r)],
            ez_s.at[x, target],
            ez_r.at[x, source],
            fs=target,
        )

    def weight_rep(x, source, owner, target):
        block = weights[x][1].at[piece(source, owner)]
        return remote(
            block, block, ep_s.at[x, source, target], ep_r.at[x, source, owner], rep=target
        )

    own_copies = [
        pltpu.make_async_copy(basis.at[c], basis_all.at[c, own_block], local.at[0]),
        pltpu.make_async_copy(wide_query, weight_query_all.at[own_block], local.at[1]),
        pltpu.make_async_copy(wide_key, weight_key_all.at[own_block], local.at[2]),
    ]
    for copy in own_copies:
        copy.start()

    def basis_rep(source, owner, target):
        block = basis_all.at[c, piece(source, owner)]
        return remote(block, block, ap_s.at[source, target], ap_r.at[source, owner], rep=target)

    def spread_basis(i):
        source = behind(i)
        basis_fs(i, source, source).wait_recv()
        each(1, rep, lambda j: basis_rep(source, r, beside(j)).start())

    each(1, fs, spread_basis)

    def start_weight(i):
        weight_fs(0, f, ahead(i)).start()
        weight_fs(1, f, ahead(i)).start()

    each(1, fs, start_weight)

    def all_basis(i):
        source = behind(i)
        each(1, rep, lambda j: basis_rep(source, beside(j), beside(j)).wait_recv())

    each(1, fs, all_basis)
    own_copies[0].wait()

    for t in range(0, tokens, LANES):
        value = jnp.dot(
            inputs[t : t + LANES, :], basis_all[c], preferred_element_type=jnp.float32
        )
        factor[c, :, t : t + LANES] = value.T.astype(jnp.bfloat16)
    for u in range(units, per * rep):
        part_send[u] = jnp.zeros(part_send.shape[1:], jnp.bfloat16)
    factor_copy = remote(
        factor.at[c], factor.at[c], pair_s.at[0], pair_r.at[0], tp=1 - c
    )
    factor_back = remote(
        factor.at[1 - c], factor.at[1 - c], pair_s.at[0], pair_r.at[0], tp=1 - c
    )
    factor_copy.start()
    swap = remote(basis_all.at[c], basis_all.at[c], pair_s.at[1], pair_r.at[1], tp=1 - c)
    swap_back = remote(
        basis_all.at[1 - c], basis_all.at[1 - c], pair_s.at[1], pair_r.at[1], tp=1 - c
    )
    factor_back.wait_recv()
    swap.start()

    for x, cot in ((0, cot_query), (1, cot_key)):
        columns = cot.shape[1]
        width = 2 * LANES if columns % (2 * LANES) == 0 else LANES
        for n in range(0, columns, width):
            value = jnp.dot(
                factor[x], cot[:, n : n + width], preferred_element_type=jnp.float32
            ).astype(jnp.bfloat16)
            for k in range(0, width, LANES):
                part_send[x * query_units + (n + k) // LANES] = value[:, k : k + LANES]

    def group(owner):
        return pl.ds(owner * per, per)

    def part_rep(source, target):
        return remote(
            part_send.at[group(target)],
            part_recv.at[source],
            bp_s.at[target],
            bp_r.at[source],
            rep=target,
        )

    each(1, rep, lambda j: part_rep(r, beside(j)).start())
    part_recv[r] = part_send[group(r)]
    each(1, rep, lambda j: part_rep(beside(j), beside(j)).wait_recv())
    for p in range(per):
        value = part_recv[0, p].astype(jnp.float32)
        for q in range(1, rep):
            value = value + part_recv[q, p].astype(jnp.float32)
        slab[p] = value.astype(jnp.bfloat16)

    def slab_fs(source, target):
        return remote(
            slab.at[:, low_rows(target)],
            slab_recv.at[source],
            bz_s.at[target],
            bz_r.at[source],
            fs=target,
        )

    each(1, fs, lambda i: slab_fs(f, ahead(i)).start())

    def spread_weight(i):
        source = behind(i)
        for x in range(2):
            weight_fs(x, source, source).wait_recv()
            each(1, rep, lambda j: weight_rep(x, source, r, beside(j)).start())

    spread_weight(1)
    slab_recv[f] = slab[:, low_rows(f), :]
    each(1, fs, lambda i: slab_fs(behind(i), behind(i)).wait_recv())
    for p in range(per):
        value = slab_recv[0, p].astype(jnp.float32)
        for q in range(1, fs):
            value = value + slab_recv[q, p].astype(jnp.float32)
        low_all[r * per + p] = value.astype(jnp.bfloat16)

    def low_rep(owner, target):
        block = low_all.at[group(owner)]
        return remote(block, block, lp_s.at[target], lp_r.at[owner], rep=target)

    each(1, rep, lambda j: low_rep(r, beside(j)).start())
    each(1, rep, lambda j: low_rep(beside(j), beside(j)).wait_recv())

    for x, moments, direction, low_out in (
        (0, moments_query, dir_query, low_query),
        (1, moments_key, dir_key, low_key),
    ):
        total = jnp.zeros((8, LANES), jnp.float32)
        for n in range(0, moments.shape[2], LANES):
            span = slice(n, n + LANES)
            low = low_all[x * query_units + n // LANES].astype(jnp.float32)
            low_out[:, span] = low
            first = 0.9 * moments[0, :, span] + 0.1 * low
            second = 0.95 * moments[1, :, span] + 0.05 * low * low
            normed = first / (jnp.sqrt(second) + 1e-08)
            direction[low_rows(f), span] = normed.astype(jnp.bfloat16)
            total = total + jnp.sum((normed * normed).reshape(rows // 8, 8, LANES), axis=0)
        squares[f, x] = total

    directions = (dir_query, dir_key)

    def direction_fs(x, source, target):
        block = directions[x].at[low_rows(source)]
        return remote(block, block, dz_s.at[x, target], dz_r.at[x, source], fs=target)

    def squares_fs(source, target):
        block = squares.at[source]
        return remote(block, block, qz_s.at[target], qz_r.at[source], fs=target)

    def start_direction(i):
        squares_fs(f, ahead(i)).start()
        direction_fs(0, f, ahead(i)).start()
        direction_fs(1, f, ahead(i)).start()

    each(1, fs, start_direction)
    each(2, fs, spread_weight)

    each(1, fs, lambda i: squares_fs(behind(i), behind(i)).wait_recv())
    total = squares[0]
    for q in range(1, fs):
        total = total + squares[q]
    pair[c] = total
    total_copy = remote(pair.at[c], pair.at[c], pair_s.at[2], pair_r.at[2], tp=1 - c)
    total_back = remote(pair.at[1 - c], pair.at[1 - c], pair_s.at[2], pair_r.at[2], tp=1 - c)
    total_copy.start()
    total_back.wait_recv()
    totals[...] = pair[0] + pair[1]

    def end_fs(i):
        source, target = behind(i), ahead(i)
        for x in range(2):
            direction_fs(x, source, source).wait_recv()
            each(1, rep, lambda j: weight_rep(x, source, beside(j), beside(j)).wait_recv())
            each(1, rep, lambda j: weight_rep(x, source, r, beside(j)).wait_send())
            weight_fs(x, f, target).wait_send()
            direction_fs(x, f, target).wait_send()
        each(1, rep, lambda j: basis_rep(source, r, beside(j)).wait_send())
        basis_fs(i, f, target).wait_send()
        slab_fs(f, target).wait_send()
        squares_fs(f, target).wait_send()

    def end_rep(j):
        part_rep(r, beside(j)).wait_send()
        low_rep(r, beside(j)).wait_send()

    each(1, fs, end_fs)
    each(1, rep, end_rep)
    swap_back.wait_recv()
    factor_copy.wait_send()
    swap.wait_send()
    total_copy.wait_send()
    own_copies[1].wait()
    own_copies[2].wait()


def on_device(
    inputs,
    cot_query,
    cot_key,
    basis_query,
    basis_key,
    weight_query,
    weight_key,
    moments_query,
    moments_key,
):
    fs, rep, tp = lax.axis_size("fs"), lax.axis_size("rep"), lax.axis_size("tp")
    assert tp == 2
    height, rank = basis_query.shape
    rows = rank // fs
    tokens = inputs.shape[0]
    query_cols, key_cols = cot_query.shape[1], cot_key.shape[1]
    per = -(-((query_cols + key_cols) // LANES) // rep)
    basis = jnp.stack([basis_query, basis_key])
    vmem = pl.BlockSpec(memory_space=pltpu.VMEM)
    hbm = pl.BlockSpec(memory_space=pl.ANY)
    bf16, f32 = jnp.bfloat16, jnp.float32
    dma = pltpu.SemaphoreType.DMA
    shape = jax.ShapeDtypeStruct
    (
        basis_all,
        weight_query_all,
        weight_key_all,
        dir_query,
        dir_key,
        low_query,
        low_key,
        totals,
    ) = pl.pallas_call(
        functools.partial(exchange, fs, rep),
        out_shape=(
            shape((2, height * fs, rank), bf16),
            shape((height * fs, query_cols), bf16),
            shape((height * fs, key_cols), bf16),
            shape((rank, query_cols), bf16),
            shape((rank, key_cols), bf16),
            shape((rows, query_cols), f32),
            shape((rows, key_cols), f32),
            shape((2, 8, LANES), f32),
        ),
        in_specs=[vmem] * 8,
        out_specs=(vmem, hbm, hbm, vmem, vmem, vmem, vmem, vmem),
        scratch_shapes=[
            pltpu.VMEM((2, rank, tokens), bf16),
            pltpu.VMEM((per * rep, rank, LANES), bf16),
            pltpu.VMEM((rep, per, rank, LANES), bf16),
            pltpu.VMEM((per, rank, LANES), bf16),
            pltpu.VMEM((fs, per, rows, LANES), bf16),
            pltpu.VMEM((per * rep, rows, LANES), bf16),
            pltpu.VMEM((fs, 2, 8, LANES), f32),
            pltpu.VMEM((2, 2, 8, LANES), f32),
            dma((fs,)),
            dma((fs,)),
            dma((fs, rep)),
            dma((fs, rep)),
            dma((2, fs)),
            dma((2, fs)),
            dma((2, fs, rep)),
            dma((2, fs, rep)),
            dma((rep,)),
            dma((rep,)),
            dma((fs,)),
            dma((fs,)),
            dma((rep,)),
            dma((rep,)),
            dma((2, fs)),
            dma((2, fs)),
            dma((fs,)),
            dma((fs,)),
            dma((3,)),
            dma((3,)),
            dma((3,)),
        ],
        compiler_params=pltpu.CompilerParams(
            collective_id=0, has_side_effects=True, vmem_limit_bytes=48 * 1024 * 1024
        ),
    )(
        inputs,
        cot_query,
        cot_key,
        basis,
        weight_query.astype(bf16),
        weight_key.astype(bf16),
        moments_query,
        moments_key,
    )

    def finish(x, total, own_basis, direction, weight, weight_all, moments, low):
        scale = lax.rsqrt(jnp.sum(total) / (low.size * fs * tp) + 1e-06)
        step = scale * jnp.dot(own_basis, direction, preferred_element_type=f32)
        new_weight = weight - 0.02 * step
        whole = scale * jnp.dot(basis_all[x], direction, preferred_element_type=f32)
        copy = (weight_all.astype(f32) - 0.02 * whole).astype(bf16)
        first = 0.9 * moments[0] + 0.1 * low
        second = 0.95 * moments[1] + 0.05 * low * low
        return step, new_weight, copy, jnp.stack([first, second])

    query = finish(
        0, totals[0], basis_query, dir_query, weight_query, weight_query_all, moments_query, low_query
    )
    key = finish(1, totals[1], basis_key, dir_key, weight_key, weight_key_all, moments_key, low_key)
    return tuple(value for both in zip(query, key) for value in both)


def solution(mesh):
    in_specs = (
        P(("fs", "rep"), None),
        P(("fs", "rep"), "tp"),
        P(("fs", "rep"), "tp"),
        P("fs", None),
        P("fs", None),
        P("fs", "tp"),
        P("fs", "tp"),
        P(None, "fs", "tp"),
        P(None, "fs", "tp"),
    )
    out_specs = (
        P("fs", "tp"),
        P("fs", "tp"),
        P("fs", "tp"),
        P("fs", "tp"),
        P(None, "tp"),
        P(None, "tp"),
        P(None, "fs", "tp"),
        P(None, "fs", "tp"),
    )
    return jax.shard_map(
        on_device, mesh=mesh, in_specs=in_specs, out_specs=out_specs, check_vma=False
    )
```

```python
import functools
import jax
import jax.numpy as jnp
from jax import lax
from jax.experimental import pallas as pl
from jax.experimental.pallas import tpu as pltpu
from jax.sharding import PartitionSpec as P

MESH = pl.DeviceIdType.MESH
LANES = 128


def each(start, stop, body):
    if stop - start <= 4:
        for i in range(start, stop):
            body(i)
    else:
        lax.fori_loop(start, stop, lambda i, carry: (body(i), carry)[1], 0)


def remote(src, dst, send_sem, recv_sem, **device):
    return pltpu.make_async_remote_copy(
        src_ref=src,
        dst_ref=dst,
        send_sem=send_sem,
        recv_sem=recv_sem,
        device_id=device,
        device_id_type=MESH,
    )


def exchange(
    fs,
    rep,
    inputs,
    cot_query,
    cot_key,
    basis_query,
    basis_key,
    full_query,
    full_key,
    moments_query,
    moments_key,
    basis_all,
    weight_query_all,
    weight_key_all,
    dir_query,
    dir_key,
    low_query,
    low_key,
    totals,
    loaded_query,
    loaded_key,
    wide_query,
    wide_key,
    factor,
    part_send,
    part_recv,
    slab,
    slab_recv,
    low_all,
    squares,
    pair,
    az_s,
    az_r,
    ap_s,
    ap_r,
    ez_s,
    ez_r,
    ep_s,
    ep_r,
    bp_s,
    bp_r,
    bz_s,
    bz_r,
    lp_s,
    lp_r,
    dr_s,
    dl_s,
    dz_r,
    qz_s,
    qz_r,
    pair_s,
    pair_r,
    local,
):
    f, r, c = lax.axis_index("fs"), lax.axis_index("rep"), lax.axis_index("tp")
    height = basis_query.shape[0]
    part = height // rep
    rank = basis_query.shape[1]
    rows = rank // fs
    tokens = inputs.shape[0]
    per = part_send.shape[0] // rep
    query_units = cot_query.shape[1] // LANES
    units = query_units + cot_key.shape[1] // LANES

    def ahead(i):
        return lax.rem(f + i, fs)

    def behind(i):
        return lax.rem(f + fs - i, fs)

    def beside(j):
        return lax.rem(r + j, rep)

    near = r + 1 - 2 * lax.rem(r, 2)
    far = r + 2 - 4 * (r // 2)
    across = 3 - r
    owners = (r, r, near, far)
    targets = (near, far, far, near)
    senders = (near, far, across, across)

    def span_of(slot, width):
        return (pl.ds(0, width), pl.ds(0, width), pl.ds(0, width // 2), pl.ds(width // 2, width // 2))[slot]

    def piece(source, owner):
        return pl.ds(pl.multiple_of(source * height + owner * part, part), part)

    own_part = pl.ds(pl.multiple_of(r * part, part), part)
    own_block = pl.ds(pl.multiple_of(f * height, height), height)

    def low_rows(source):
        return pl.ds(pl.multiple_of(source * rows, rows), rows)

    loads = [
        pltpu.make_async_copy(full_query, loaded_query, local.at[3]),
        pltpu.make_async_copy(full_key, loaded_key, local.at[4]),
    ]
    for load in loads:
        load.start()
    barrier = pltpu.get_barrier_semaphore()

    def greet_fs(i):
        pl.semaphore_signal(barrier, inc=1, device_id={"fs": ahead(i)}, device_id_type=MESH)

    def greet_rep(j):
        pl.semaphore_signal(barrier, inc=1, device_id={"rep": beside(j)}, device_id_type=MESH)

    each(1, fs, greet_fs)
    each(1, rep, greet_rep)
    pl.semaphore_signal(barrier, inc=1, device_id={"tp": 1 - c}, device_id_type=MESH)
    pl.semaphore_wait(barrier, fs + rep - 1)

    bases = (basis_query, basis_key)
    weights = ((wide_query, weight_query_all), (wide_key, weight_key_all))

    def basis_fs(x, source, target):
        return remote(
            bases[x].at[own_part],
            basis_all.at[c, piece(source, r)],
            az_s.at[target],
            az_r.at[source],
            fs=target,
        )

    for x in range(2):

        @pl.when(c == x)
        def start_basis():
            each(1, fs, lambda i: basis_fs(x, f, ahead(i)).start())
            pltpu.make_async_copy(bases[x], basis_all.at[c, own_block], local.at[0]).start()

    own_basis = pltpu.make_async_copy(basis_query, basis_all.at[c, own_block], local.at[0])

    def basis_hop(source, slot, owner):
        block = basis_all.at[c, piece(source, owner), span_of(slot, rank)]
        return remote(
            block, block, ap_s.at[source, slot], ap_r.at[source, slot], rep=targets[slot]
        )

    def weight_fs(x, source, target):
        return remote(
            weights[x][0].at[own_part],
            weights[x][1].at[piece(source, r)],
            ez_s.at[x, target],
            ez_r.at[x, source],
            fs=target,
        )

    def weight_hop(x, source, slot, owner):
        block = weights[x][1].at[piece(source, owner), span_of(slot, weights[x][1].shape[1])]
        return remote(
            block, block, ep_s.at[x, source, slot], ep_r.at[x, source, slot], rep=targets[slot]
        )

    for load in loads:
        load.wait()
    wide_query[...] = loaded_query[...].astype(jnp.bfloat16)
    wide_key[...] = loaded_key[...].astype(jnp.bfloat16)

    def spread_basis(i):
        source = behind(i)
        basis_fs(0, source, source).wait_recv()
        for slot in (0, 1):
            basis_hop(source, slot, owners[slot]).start()

    each(1, fs, spread_basis)

    own_copies = [
        pltpu.make_async_copy(wide_query, weight_query_all.at[own_block], local.at[1]),
        pltpu.make_async_copy(wide_key, weight_key_all.at[own_block], local.at[2]),
    ]
    for copy in own_copies:
        copy.start()

    def start_weight(i):
        weight_fs(0, f, ahead(i)).start()
        weight_fs(1, f, ahead(i)).start()

    each(1, fs, start_weight)

    def relay_basis(i):
        source = behind(i)
        for slot in (0, 1):
            basis_hop(source, slot, senders[slot]).wait_recv()
            basis_hop(source, slot + 2, owners[slot + 2]).start()

    def all_basis(i):
        for slot in (2, 3):
            basis_hop(behind(i), slot, senders[slot]).wait_recv()

    each(1, fs, relay_basis)
    each(1, fs, all_basis)
    own_basis.wait()

    for t in range(0, tokens, LANES):
        value = jnp.dot(
            inputs[t : t + LANES, :], basis_all[c], preferred_element_type=jnp.float32
        )
        factor[c, :, t : t + LANES] = value.T.astype(jnp.bfloat16)
    for u in range(units, per * rep):
        part_send[u] = jnp.zeros(part_send.shape[1:], jnp.bfloat16)
    factor_copy = remote(
        factor.at[c], factor.at[c], pair_s.at[0], pair_r.at[0], tp=1 - c
    )
    factor_back = remote(
        factor.at[1 - c], factor.at[1 - c], pair_s.at[0], pair_r.at[0], tp=1 - c
    )
    factor_copy.start()
    swap = remote(basis_all.at[c], basis_all.at[c], pair_s.at[1], pair_r.at[1], tp=1 - c)
    swap_back = remote(
        basis_all.at[1 - c], basis_all.at[1 - c], pair_s.at[1], pair_r.at[1], tp=1 - c
    )
    factor_back.wait_recv()
    swap.start()

    for x, cot in ((0, cot_query), (1, cot_key)):
        columns = cot.shape[1]
        width = 2 * LANES if columns % (2 * LANES) == 0 else LANES
        for n in range(0, columns, width):
            value = jnp.dot(
                factor[x], cot[:, n : n + width], preferred_element_type=jnp.float32
            ).astype(jnp.bfloat16)
            for k in range(0, width, LANES):
                part_send[x * query_units + (n + k) // LANES] = value[:, k : k + LANES]

    def group(owner):
        return pl.ds(owner * per, per)

    def part_rep(source, target):
        return remote(
            part_send.at[group(target)],
            part_recv.at[source],
            bp_s.at[target],
            bp_r.at[source],
            rep=target,
        )

    each(1, rep, lambda j: part_rep(r, beside(j)).start())
    part_recv[r] = part_send[group(r)]
    each(1, rep, lambda j: part_rep(beside(j), beside(j)).wait_recv())
    for p in range(per):
        value = part_recv[0, p].astype(jnp.float32)
        for q in range(1, rep):
            value = value + part_recv[q, p].astype(jnp.float32)
        slab[p] = value.astype(jnp.bfloat16)

    def slab_fs(source, target):
        return remote(
            slab.at[:, low_rows(target)],
            slab_recv.at[source],
            bz_s.at[target],
            bz_r.at[source],
            fs=target,
        )

    each(1, fs, lambda i: slab_fs(f, ahead(i)).start())

    def spread_weight(i):
        source = behind(i)
        for x in range(2):
            weight_fs(x, source, source).wait_recv()
            for slot in (0, 1):
                weight_hop(x, source, slot, owners[slot]).start()

    def relay_weight(i):
        source = behind(i)
        for slot in (0, 1):
            for x in range(2):
                weight_hop(x, source, slot, senders[slot]).wait_recv()
                weight_hop(x, source, slot + 2, owners[slot + 2]).start()

    spread_weight(1)
    slab_recv[f] = slab[:, low_rows(f), :]
    each(1, fs, lambda i: slab_fs(behind(i), behind(i)).wait_recv())
    for p in range(per):
        value = slab_recv[0, p].astype(jnp.float32)
        for q in range(1, fs):
            value = value + slab_recv[q, p].astype(jnp.float32)
        low_all[r * per + p] = value.astype(jnp.bfloat16)

    def low_rep(owner, target):
        block = low_all.at[group(owner)]
        return remote(block, block, lp_s.at[target], lp_r.at[owner], rep=target)

    each(1, rep, lambda j: low_rep(r, beside(j)).start())
    each(1, rep, lambda j: low_rep(beside(j), beside(j)).wait_recv())

    for x, moments, direction, low_out in (
        (0, moments_query, dir_query, low_query),
        (1, moments_key, dir_key, low_key),
    ):
        total = jnp.zeros((8, LANES), jnp.float32)
        for n in range(0, moments.shape[2], LANES):
            span = slice(n, n + LANES)
            low = low_all[x * query_units + n // LANES].astype(jnp.float32)
            low_out[:, span] = low
            first = 0.9 * moments[0, :, span] + 0.1 * low
            second = 0.95 * moments[1, :, span] + 0.05 * low * low
            normed = first / (jnp.sqrt(second) + 1e-08)
            direction[low_rows(f), span] = normed.astype(jnp.bfloat16)
            total = total + jnp.sum((normed * normed).reshape(rows // 8, 8, LANES), axis=0)
        squares[f, x] = total

    directions = (dir_query, dir_key)

    right, left = ahead(1), behind(1)

    def move_right(x, source):
        block = directions[x].at[low_rows(source)]
        return remote(block, block, dr_s.at[x, source], dz_r.at[x, source], fs=right)

    def move_left(x, source):
        block = directions[x].at[low_rows(source)]
        return remote(block, block, dl_s.at[x, source], dz_r.at[x, source], fs=left)

    def squares_fs(source, target):
        block = squares.at[source]
        return remote(block, block, qz_s.at[target], qz_r.at[source], fs=target)

    each(1, fs, lambda i: squares_fs(f, ahead(i)).start())

    @pl.when(f + 1 < fs)
    def start_right():
        for x in range(2):
            move_right(x, f).start()

    @pl.when(f > 0)
    def start_left():
        for x in range(2):
            move_left(x, f).start()

    each(2, fs, spread_weight)

    def relay_direction(k):
        @pl.when(f - k >= 0)
        def from_left():
            for x in range(2):
                move_right(x, f - k).wait_recv()

                @pl.when(f + 1 < fs)
                def onward():
                    move_right(x, f - k).start()

        @pl.when(f + k < fs)
        def from_right():
            for x in range(2):
                move_left(x, f + k).wait_recv()

                @pl.when(f > 0)
                def onward():
                    move_left(x, f + k).start()

    def relay_both(k):
        relay_weight(k)
        relay_direction(k)

    each(1, fs, relay_both)

    each(1, fs, lambda i: squares_fs(behind(i), behind(i)).wait_recv())
    total = squares[0]
    for q in range(1, fs):
        total = total + squares[q]
    pair[c] = total
    total_copy = remote(pair.at[c], pair.at[c], pair_s.at[2], pair_r.at[2], tp=1 - c)
    total_back = remote(pair.at[1 - c], pair.at[1 - c], pair_s.at[2], pair_r.at[2], tp=1 - c)
    total_copy.start()
    total_back.wait_recv()
    totals[...] = pair[0] + pair[1]

    def end_fs(i):
        source, target = behind(i), ahead(i)
        for x in range(2):
            for slot in (2, 3):
                weight_hop(x, source, slot, senders[slot]).wait_recv()
            for slot in range(4):
                weight_hop(x, source, slot, owners[slot]).wait_send()
            weight_fs(x, f, target).wait_send()
        for slot in range(4):
            basis_hop(source, slot, owners[slot]).wait_send()
        basis_fs(0, f, target).wait_send()
        slab_fs(f, target).wait_send()
        squares_fs(f, target).wait_send()

    def end_direction(k):
        @pl.when((f - k >= 0) & (f + 1 < fs))
        def end_right():
            for x in range(2):
                move_right(x, f - k).wait_send()

        @pl.when((f + k < fs) & (f > 0))
        def end_left():
            for x in range(2):
                move_left(x, f + k).wait_send()

    def end_rep(j):
        part_rep(r, beside(j)).wait_send()
        low_rep(r, beside(j)).wait_send()

    each(1, fs, end_fs)
    each(0, fs, end_direction)
    each(1, rep, end_rep)
    swap_back.wait_recv()
    factor_copy.wait_send()
    swap.wait_send()
    total_copy.wait_send()
    for copy in own_copies:
        copy.wait()


def apply(
    count_query,
    count_key,
    totals,
    dir_query,
    dir_key,
    low_query,
    low_key,
    moments_query,
    moments_key,
    basis_all,
    weight_query_all,
    weight_key_all,
    basis_query,
    basis_key,
    weight_query,
    weight_key,
    step_query,
    step_key,
    new_weight_query,
    new_weight_key,
    copy_query,
    copy_key,
    new_moments_query,
    new_moments_key,
):
    parts = (
        (count_query, dir_query, weight_query_all, basis_query, weight_query),
        (count_key, dir_key, weight_key_all, basis_key, weight_key),
    )
    outs = (
        (step_query, new_weight_query, copy_query),
        (step_key, new_weight_key, copy_key),
    )
    for x in range(2):
        count, direction, weight_all, basis, weight = parts[x]
        step_out, new_weight_out, copy_out = outs[x]
        scale = lax.rsqrt(jnp.sum(totals[x], keepdims=True) / count + 1e-06)
        step = scale * jnp.dot(basis[...], direction[...], preferred_element_type=jnp.float32)
        step_out[...] = step
        new_weight_out[...] = weight[...] - 0.02 * step
        whole = scale * jnp.dot(
            basis_all[x], direction[...], preferred_element_type=jnp.float32
        )
        copy_out[...] = (weight_all[...].astype(jnp.float32) - 0.02 * whole).astype(jnp.bfloat16)

    @pl.when(pl.program_id(0) == 0)
    def moments_once():
        for moments, low_ref, out in (
            (moments_query, low_query, new_moments_query),
            (moments_key, low_key, new_moments_key),
        ):
            low = low_ref[...]
            out[0] = 0.9 * moments[0] + 0.1 * low
            out[1] = 0.95 * moments[1] + 0.05 * low * low


def on_device(
    inputs,
    cot_query,
    cot_key,
    basis_query,
    basis_key,
    weight_query,
    weight_key,
    moments_query,
    moments_key,
):
    fs, rep, tp = lax.axis_size("fs"), lax.axis_size("rep"), lax.axis_size("tp")
    assert tp == 2 and rep == 4
    height, rank = basis_query.shape
    rows = rank // fs
    tokens = inputs.shape[0]
    query_cols, key_cols = cot_query.shape[1], cot_key.shape[1]
    per = -(-((query_cols + key_cols) // LANES) // rep)
    vmem = pl.BlockSpec(memory_space=pltpu.VMEM)
    hbm = pl.BlockSpec(memory_space=pl.ANY)
    bf16, f32 = jnp.bfloat16, jnp.float32
    dma = pltpu.SemaphoreType.DMA
    shape = jax.ShapeDtypeStruct
    (
        basis_all,
        weight_query_all,
        weight_key_all,
        dir_query,
        dir_key,
        low_query,
        low_key,
        totals,
    ) = pl.pallas_call(
        functools.partial(exchange, fs, rep),
        out_shape=(
            shape((2, height * fs, rank), bf16),
            shape((height * fs, query_cols), bf16),
            shape((height * fs, key_cols), bf16),
            shape((rank, query_cols), bf16),
            shape((rank, key_cols), bf16),
            shape((rows, query_cols), f32),
            shape((rows, key_cols), f32),
            shape((2, 8, LANES), f32),
        ),
        in_specs=[vmem] * 5 + [hbm, hbm, vmem, vmem],
        out_specs=(vmem, hbm, hbm, vmem, vmem, vmem, vmem, vmem),
        scratch_shapes=[
            pltpu.VMEM((height, query_cols), f32),
            pltpu.VMEM((height, key_cols), f32),
            pltpu.VMEM((height, query_cols), bf16),
            pltpu.VMEM((height, key_cols), bf16),
            pltpu.VMEM((2, rank, tokens), bf16),
            pltpu.VMEM((per * rep, rank, LANES), bf16),
            pltpu.VMEM((rep, per, rank, LANES), bf16),
            pltpu.VMEM((per, rank, LANES), bf16),
            pltpu.VMEM((fs, per, rows, LANES), bf16),
            pltpu.VMEM((per * rep, rows, LANES), bf16),
            pltpu.VMEM((fs, 2, 8, LANES), f32),
            pltpu.VMEM((2, 2, 8, LANES), f32),
            dma((fs,)),
            dma((fs,)),
            dma((fs, rep)),
            dma((fs, rep)),
            dma((2, fs)),
            dma((2, fs)),
            dma((2, fs, rep)),
            dma((2, fs, rep)),
            dma((rep,)),
            dma((rep,)),
            dma((fs,)),
            dma((fs,)),
            dma((rep,)),
            dma((rep,)),
            dma((2, fs)),
            dma((2, fs)),
            dma((2, fs)),
            dma((fs,)),
            dma((fs,)),
            dma((3,)),
            dma((3,)),
            dma((5,)),
        ],
        compiler_params=pltpu.CompilerParams(
            collective_id=0, has_side_effects=True, vmem_limit_bytes=32 * 1024 * 1024
        ),
    )(
        inputs,
        cot_query,
        cot_key,
        basis_query,
        basis_key,
        weight_query,
        weight_key,
        moments_query,
        moments_key,
    )

    steps = min(8, height // 16)
    tall, short = height * fs // steps, height // steps

    def fixed(*dims):
        return pl.BlockSpec(dims, lambda i: (0,) * len(dims))

    def banded(*dims):
        return pl.BlockSpec(dims, lambda i: (i, 0))

    owned = tuple(
        shape((height, columns), f32) for columns in (query_cols, key_cols, query_cols, key_cols)
    )
    owned_specs = tuple(
        banded(short, columns) for columns in (query_cols, key_cols, query_cols, key_cols)
    )
    return pl.pallas_call(
        functools.partial(
            apply, float(rank * query_cols * tp), float(rank * key_cols * tp)
        ),
        grid=(steps,),
        out_shape=owned
        + (
            shape((height * fs, query_cols), bf16),
            shape((height * fs, key_cols), bf16),
            shape((2, rows, query_cols), f32),
            shape((2, rows, key_cols), f32),
        ),
        in_specs=[
            fixed(2, 8, LANES),
            fixed(rank, query_cols),
            fixed(rank, key_cols),
            fixed(rows, query_cols),
            fixed(rows, key_cols),
            fixed(2, rows, query_cols),
            fixed(2, rows, key_cols),
            pl.BlockSpec((2, tall, rank), lambda i: (0, i, 0)),
            banded(tall, query_cols),
            banded(tall, key_cols),
            banded(short, rank),
            banded(short, rank),
            banded(short, query_cols),
            banded(short, key_cols),
        ],
        out_specs=owned_specs
        + (
            banded(tall, query_cols),
            banded(tall, key_cols),
            fixed(2, rows, query_cols),
            fixed(2, rows, key_cols),
        ),
        compiler_params=pltpu.CompilerParams(
            dimension_semantics=("arbitrary",), vmem_limit_bytes=32 * 1024 * 1024
        ),
    )(
        totals,
        dir_query,
        dir_key,
        low_query,
        low_key,
        moments_query,
        moments_key,
        basis_all,
        weight_query_all,
        weight_key_all,
        basis_query,
        basis_key,
        weight_query,
        weight_key,
    )


def solution(mesh):
    in_specs = (
        P(("fs", "rep"), None),
        P(("fs", "rep"), "tp"),
        P(("fs", "rep"), "tp"),
        P("fs", None),
        P("fs", None),
        P("fs", "tp"),
        P("fs", "tp"),
        P(None, "fs", "tp"),
        P(None, "fs", "tp"),
    )
    out_specs = (
        P("fs", "tp"),
        P("fs", "tp"),
        P("fs", "tp"),
        P("fs", "tp"),
        P(None, "tp"),
        P(None, "tp"),
        P(None, "fs", "tp"),
        P(None, "fs", "tp"),
    )
    return jax.shard_map(
        on_device, mesh=mesh, in_specs=in_specs, out_specs=out_specs, check_vma=False
    )
```

```python
import functools
import jax
import jax.numpy as jnp
from jax import lax
from jax.experimental import pallas as pl
from jax.experimental.pallas import tpu as pltpu
from jax.sharding import PartitionSpec as P

MESH = pl.DeviceIdType.MESH
LANES = 128


def each(start, stop, body):
    if stop - start <= 4:
        for i in range(start, stop):
            body(i)
    else:
        lax.fori_loop(start, stop, lambda i, carry: (body(i), carry)[1], 0)


def remote(src, dst, send_sem, recv_sem, **device):
    return pltpu.make_async_remote_copy(
        src_ref=src,
        dst_ref=dst,
        send_sem=send_sem,
        recv_sem=recv_sem,
        device_id=device,
        device_id_type=MESH,
    )


def exchange(
    fs,
    rep,
    inputs_far,
    cot_query_far,
    cot_key_far,
    basis_query,
    basis_key,
    full_query,
    full_key,
    moments_query_far,
    moments_key_far,
    basis_all,
    weight_query_all,
    weight_key_all,
    dir_query,
    dir_key,
    low_query,
    low_key,
    totals,
    inputs,
    cot_query,
    cot_key,
    moments_query,
    moments_key,
    loaded_query,
    loaded_key,
    wide_query,
    wide_key,
    factor,
    part_send,
    part_recv,
    slab,
    slab_recv,
    low_all,
    squares,
    pair,
    az_s,
    az_r,
    ap_s,
    ap_r,
    ez_s,
    ez_r,
    ep_s,
    ep_r,
    bp_s,
    bp_r,
    bz_s,
    bz_r,
    lp_s,
    lp_r,
    dr_s,
    dl_s,
    dz_r,
    qz_s,
    qz_r,
    pair_s,
    pair_r,
    local,
):
    f, r, c = lax.axis_index("fs"), lax.axis_index("rep"), lax.axis_index("tp")
    height = basis_query.shape[0]
    part = height // rep
    rank = basis_query.shape[1]
    rows = rank // fs
    tokens = inputs.shape[0]
    per = part_send.shape[0] // rep
    query_units = cot_query.shape[1] // LANES
    units = query_units + cot_key.shape[1] // LANES

    def ahead(i):
        return lax.rem(f + i, fs)

    def behind(i):
        return lax.rem(f + fs - i, fs)

    def beside(j):
        return lax.rem(r + j, rep)

    near = r + 1 - 2 * lax.rem(r, 2)
    far = r + 2 - 4 * (r // 2)
    across = 3 - r
    owners = (r, r, near, far)
    targets = (near, far, far, near)
    senders = (near, far, across, across)

    def span_of(slot, width):
        return (pl.ds(0, width), pl.ds(0, width), pl.ds(0, width // 2), pl.ds(width // 2, width // 2))[slot]

    def piece(source, owner):
        return pl.ds(pl.multiple_of(source * height + owner * part, part), part)

    own_part = pl.ds(pl.multiple_of(r * part, part), part)
    own_block = pl.ds(pl.multiple_of(f * height, height), height)

    def low_rows(source):
        return pl.ds(pl.multiple_of(source * rows, rows), rows)

    loads = [
        pltpu.make_async_copy(source, target, local.at[3 + n])
        for n, (source, target) in enumerate(
            (
                (full_query, loaded_query),
                (full_key, loaded_key),
                (inputs_far, inputs),
                (cot_query_far, cot_query),
                (cot_key_far, cot_key),
                (moments_query_far, moments_query),
                (moments_key_far, moments_key),
            )
        )
    ]
    barrier = pltpu.get_barrier_semaphore()

    def greet_fs(i):
        pl.semaphore_signal(barrier, inc=1, device_id={"fs": ahead(i)}, device_id_type=MESH)

    def greet_rep(j):
        pl.semaphore_signal(barrier, inc=1, device_id={"rep": beside(j)}, device_id_type=MESH)

    each(1, fs, greet_fs)
    each(1, rep, greet_rep)
    pl.semaphore_signal(barrier, inc=1, device_id={"tp": 1 - c}, device_id_type=MESH)
    pl.semaphore_wait(barrier, fs + rep - 1)

    bases = (basis_query, basis_key)
    weights = ((wide_query, weight_query_all), (wide_key, weight_key_all))

    def basis_fs(x, source, target):
        return remote(
            bases[x].at[own_part],
            basis_all.at[c, piece(source, r)],
            az_s.at[target],
            az_r.at[source],
            fs=target,
        )

    for x in range(2):

        @pl.when(c == x)
        def start_basis():
            each(1, fs, lambda i: basis_fs(x, f, ahead(i)).start())
            pltpu.make_async_copy(bases[x], basis_all.at[c, own_block], local.at[0]).start()

    for load in loads:
        load.start()
    own_basis = pltpu.make_async_copy(basis_query, basis_all.at[c, own_block], local.at[0])

    def basis_hop(source, slot, owner):
        block = basis_all.at[c, piece(source, owner), span_of(slot, rank)]
        return remote(
            block, block, ap_s.at[source, slot], ap_r.at[source, slot], rep=targets[slot]
        )

    def weight_fs(x, source, target):
        return remote(
            weights[x][0].at[own_part],
            weights[x][1].at[piece(source, r)],
            ez_s.at[x, target],
            ez_r.at[x, source],
            fs=target,
        )

    def weight_hop(x, source, slot, owner):
        block = weights[x][1].at[piece(source, owner), span_of(slot, weights[x][1].shape[1])]
        return remote(
            block, block, ep_s.at[x, source, slot], ep_r.at[x, source, slot], rep=targets[slot]
        )

    for load in loads[:2]:
        load.wait()
    wide_query[...] = loaded_query[...].astype(jnp.bfloat16)
    wide_key[...] = loaded_key[...].astype(jnp.bfloat16)

    def spread_basis(i):
        source = behind(i)
        basis_fs(0, source, source).wait_recv()
        for slot in (0, 1):
            basis_hop(source, slot, owners[slot]).start()

    each(1, fs, spread_basis)

    own_copies = [
        pltpu.make_async_copy(wide_query, weight_query_all.at[own_block], local.at[1]),
        pltpu.make_async_copy(wide_key, weight_key_all.at[own_block], local.at[2]),
    ]
    for copy in own_copies:
        copy.start()

    def start_weight(i):
        weight_fs(0, f, ahead(i)).start()
        weight_fs(1, f, ahead(i)).start()

    each(1, fs, start_weight)

    def relay_basis(i):
        source = behind(i)
        for slot in (0, 1):
            basis_hop(source, slot, senders[slot]).wait_recv()
            basis_hop(source, slot + 2, owners[slot + 2]).start()

    def all_basis(i):
        for slot in (2, 3):
            basis_hop(behind(i), slot, senders[slot]).wait_recv()

    each(1, fs, relay_basis)
    each(1, fs, all_basis)
    own_basis.wait()
    for load in loads[2:]:
        load.wait()

    for t in range(0, tokens, LANES):
        value = jnp.dot(
            inputs[t : t + LANES, :], basis_all[c], preferred_element_type=jnp.float32
        )
        factor[c, :, t : t + LANES] = value.T.astype(jnp.bfloat16)
    for u in range(units, per * rep):
        part_send[u] = jnp.zeros(part_send.shape[1:], jnp.bfloat16)
    factor_copy = remote(
        factor.at[c], factor.at[c], pair_s.at[0], pair_r.at[0], tp=1 - c
    )
    factor_back = remote(
        factor.at[1 - c], factor.at[1 - c], pair_s.at[0], pair_r.at[0], tp=1 - c
    )
    factor_copy.start()
    swap = remote(basis_all.at[c], basis_all.at[c], pair_s.at[1], pair_r.at[1], tp=1 - c)
    swap_back = remote(
        basis_all.at[1 - c], basis_all.at[1 - c], pair_s.at[1], pair_r.at[1], tp=1 - c
    )
    factor_back.wait_recv()
    swap.start()

    for x, cot in ((0, cot_query), (1, cot_key)):
        columns = cot.shape[1]
        width = 2 * LANES if columns % (2 * LANES) == 0 else LANES
        for n in range(0, columns, width):
            value = jnp.dot(
                factor[x], cot[:, n : n + width], preferred_element_type=jnp.float32
            ).astype(jnp.bfloat16)
            for k in range(0, width, LANES):
                part_send[x * query_units + (n + k) // LANES] = value[:, k : k + LANES]

    def group(owner):
        return pl.ds(owner * per, per)

    def part_rep(source, target):
        return remote(
            part_send.at[group(target)],
            part_recv.at[source],
            bp_s.at[target],
            bp_r.at[source],
            rep=target,
        )

    each(1, rep, lambda j: part_rep(r, beside(j)).start())
    part_recv[r] = part_send[group(r)]
    each(1, rep, lambda j: part_rep(beside(j), beside(j)).wait_recv())
    for p in range(per):
        value = part_recv[0, p].astype(jnp.float32)
        for q in range(1, rep):
            value = value + part_recv[q, p].astype(jnp.float32)
        slab[p] = value.astype(jnp.bfloat16)

    def slab_fs(source, target):
        return remote(
            slab.at[:, low_rows(target)],
            slab_recv.at[source],
            bz_s.at[target],
            bz_r.at[source],
            fs=target,
        )

    each(1, fs, lambda i: slab_fs(f, ahead(i)).start())

    def spread_weight(i):
        source = behind(i)
        for x in range(2):
            weight_fs(x, source, source).wait_recv()
            for slot in (0, 1):
                weight_hop(x, source, slot, owners[slot]).start()

    def relay_weight(i):
        source = behind(i)
        for slot in (0, 1):
            for x in range(2):
                weight_hop(x, source, slot, senders[slot]).wait_recv()
                weight_hop(x, source, slot + 2, owners[slot + 2]).start()

    spread_weight(1)
    slab_recv[f] = slab[:, low_rows(f), :]
    each(1, fs, lambda i: slab_fs(behind(i), behind(i)).wait_recv())
    for p in range(per):
        value = slab_recv[0, p].astype(jnp.float32)
        for q in range(1, fs):
            value = value + slab_recv[q, p].astype(jnp.float32)
        low_all[r * per + p] = value.astype(jnp.bfloat16)

    def low_rep(owner, target):
        block = low_all.at[group(owner)]
        return remote(block, block, lp_s.at[target], lp_r.at[owner], rep=target)

    each(1, rep, lambda j: low_rep(r, beside(j)).start())
    each(1, rep, lambda j: low_rep(beside(j), beside(j)).wait_recv())

    for x, moments, direction, low_out in (
        (0, moments_query, dir_query, low_query),
        (1, moments_key, dir_key, low_key),
    ):
        total = jnp.zeros((8, LANES), jnp.float32)
        for n in range(0, moments.shape[2], LANES):
            span = slice(n, n + LANES)
            low = low_all[x * query_units + n // LANES].astype(jnp.float32)
            low_out[:, span] = low
            first = 0.9 * moments[0, :, span] + 0.1 * low
            second = 0.95 * moments[1, :, span] + 0.05 * low * low
            normed = first / (jnp.sqrt(second) + 1e-08)
            direction[low_rows(f), span] = normed.astype(jnp.bfloat16)
            total = total + jnp.sum((normed * normed).reshape(rows // 8, 8, LANES), axis=0)
        squares[f, x] = total

    directions = (dir_query, dir_key)

    right, left = ahead(1), behind(1)

    def move_right(x, source):
        block = directions[x].at[low_rows(source)]
        return remote(block, block, dr_s.at[x, source], dz_r.at[x, source], fs=right)

    def move_left(x, source):
        block = directions[x].at[low_rows(source)]
        return remote(block, block, dl_s.at[x, source], dz_r.at[x, source], fs=left)

    def squares_fs(source, target):
        block = squares.at[source]
        return remote(block, block, qz_s.at[target], qz_r.at[source], fs=target)

    each(1, fs, lambda i: squares_fs(f, ahead(i)).start())

    @pl.when(f + 1 < fs)
    def start_right():
        for x in range(2):
            move_right(x, f).start()

    @pl.when(f > 0)
    def start_left():
        for x in range(2):
            move_left(x, f).start()

    each(2, fs, spread_weight)

    def relay_direction(k):
        @pl.when(f - k >= 0)
        def from_left():
            for x in range(2):
                move_right(x, f - k).wait_recv()

                @pl.when(f + 1 < fs)
                def onward():
                    move_right(x, f - k).start()

        @pl.when(f + k < fs)
        def from_right():
            for x in range(2):
                move_left(x, f + k).wait_recv()

                @pl.when(f > 0)
                def onward():
                    move_left(x, f + k).start()

    def relay_both(k):
        relay_weight(k)
        relay_direction(k)

    each(1, fs, relay_both)

    each(1, fs, lambda i: squares_fs(behind(i), behind(i)).wait_recv())
    total = squares[0]
    for q in range(1, fs):
        total = total + squares[q]
    pair[c] = total
    total_copy = remote(pair.at[c], pair.at[c], pair_s.at[2], pair_r.at[2], tp=1 - c)
    total_back = remote(pair.at[1 - c], pair.at[1 - c], pair_s.at[2], pair_r.at[2], tp=1 - c)
    total_copy.start()
    total_back.wait_recv()
    totals[...] = pair[0] + pair[1]

    def end_fs(i):
        source, target = behind(i), ahead(i)
        for x in range(2):
            for slot in (2, 3):
                weight_hop(x, source, slot, senders[slot]).wait_recv()
            for slot in range(4):
                weight_hop(x, source, slot, owners[slot]).wait_send()
            weight_fs(x, f, target).wait_send()
        for slot in range(4):
            basis_hop(source, slot, owners[slot]).wait_send()
        basis_fs(0, f, target).wait_send()
        slab_fs(f, target).wait_send()
        squares_fs(f, target).wait_send()

    def end_direction(k):
        @pl.when((f - k >= 0) & (f + 1 < fs))
        def end_right():
            for x in range(2):
                move_right(x, f - k).wait_send()

        @pl.when((f + k < fs) & (f > 0))
        def end_left():
            for x in range(2):
                move_left(x, f + k).wait_send()

    def end_rep(j):
        part_rep(r, beside(j)).wait_send()
        low_rep(r, beside(j)).wait_send()

    each(1, fs, end_fs)
    each(0, fs, end_direction)
    each(1, rep, end_rep)
    swap_back.wait_recv()
    factor_copy.wait_send()
    swap.wait_send()
    total_copy.wait_send()
    for copy in own_copies:
        copy.wait()


def apply(
    count_query,
    count_key,
    totals,
    dir_query,
    dir_key,
    low_query,
    low_key,
    moments_query,
    moments_key,
    basis_all,
    weight_query_all,
    weight_key_all,
    basis_query,
    basis_key,
    weight_query,
    weight_key,
    step_query,
    step_key,
    new_weight_query,
    new_weight_key,
    copy_query,
    copy_key,
    new_moments_query,
    new_moments_key,
):
    parts = (
        (count_query, dir_query, weight_query_all, basis_query, weight_query),
        (count_key, dir_key, weight_key_all, basis_key, weight_key),
    )
    outs = (
        (step_query, new_weight_query, copy_query),
        (step_key, new_weight_key, copy_key),
    )
    for x in range(2):
        count, direction, weight_all, basis, weight = parts[x]
        step_out, new_weight_out, copy_out = outs[x]
        scale = lax.rsqrt(jnp.sum(totals[x], keepdims=True) / count + 1e-06)
        step = scale * jnp.dot(basis[...], direction[...], preferred_element_type=jnp.float32)
        step_out[...] = step
        new_weight_out[...] = weight[...] - 0.02 * step
        whole = scale * jnp.dot(
            basis_all[x], direction[...], preferred_element_type=jnp.float32
        )
        copy_out[...] = (weight_all[...].astype(jnp.float32) - 0.02 * whole).astype(jnp.bfloat16)

    @pl.when(pl.program_id(0) == 0)
    def moments_once():
        for moments, low_ref, out in (
            (moments_query, low_query, new_moments_query),
            (moments_key, low_key, new_moments_key),
        ):
            low = low_ref[...]
            out[0] = 0.9 * moments[0] + 0.1 * low
            out[1] = 0.95 * moments[1] + 0.05 * low * low


def on_device(
    inputs,
    cot_query,
    cot_key,
    basis_query,
    basis_key,
    weight_query,
    weight_key,
    moments_query,
    moments_key,
):
    fs, rep, tp = lax.axis_size("fs"), lax.axis_size("rep"), lax.axis_size("tp")
    assert tp == 2 and rep == 4
    height, rank = basis_query.shape
    rows = rank // fs
    tokens = inputs.shape[0]
    query_cols, key_cols = cot_query.shape[1], cot_key.shape[1]
    per = -(-((query_cols + key_cols) // LANES) // rep)
    vmem = pl.BlockSpec(memory_space=pltpu.VMEM)
    hbm = pl.BlockSpec(memory_space=pl.ANY)
    bf16, f32 = jnp.bfloat16, jnp.float32
    dma = pltpu.SemaphoreType.DMA
    shape = jax.ShapeDtypeStruct
    (
        basis_all,
        weight_query_all,
        weight_key_all,
        dir_query,
        dir_key,
        low_query,
        low_key,
        totals,
    ) = pl.pallas_call(
        functools.partial(exchange, fs, rep),
        out_shape=(
            shape((2, height * fs, rank), bf16),
            shape((height * fs, query_cols), bf16),
            shape((height * fs, key_cols), bf16),
            shape((rank, query_cols), bf16),
            shape((rank, key_cols), bf16),
            shape((rows, query_cols), f32),
            shape((rows, key_cols), f32),
            shape((2, 8, LANES), f32),
        ),
        in_specs=[pl.BlockSpec(memory_space=pltpu.HBM)] * 9,
        out_specs=(vmem, hbm, hbm, vmem, vmem, vmem, vmem, vmem),
        scratch_shapes=[
            pltpu.VMEM((tokens, inputs.shape[1]), bf16),
            pltpu.VMEM((tokens, query_cols), bf16),
            pltpu.VMEM((tokens, key_cols), bf16),
            pltpu.VMEM((2, rows, query_cols), f32),
            pltpu.VMEM((2, rows, key_cols), f32),
            pltpu.VMEM((height, query_cols), f32),
            pltpu.VMEM((height, key_cols), f32),
            pltpu.VMEM((height, query_cols), bf16),
            pltpu.VMEM((height, key_cols), bf16),
            pltpu.VMEM((2, rank, tokens), bf16),
            pltpu.VMEM((per * rep, rank, LANES), bf16),
            pltpu.VMEM((rep, per, rank, LANES), bf16),
            pltpu.VMEM((per, rank, LANES), bf16),
            pltpu.VMEM((fs, per, rows, LANES), bf16),
            pltpu.VMEM((per * rep, rows, LANES), bf16),
            pltpu.VMEM((fs, 2, 8, LANES), f32),
            pltpu.VMEM((2, 2, 8, LANES), f32),
            dma((fs,)),
            dma((fs,)),
            dma((fs, rep)),
            dma((fs, rep)),
            dma((2, fs)),
            dma((2, fs)),
            dma((2, fs, rep)),
            dma((2, fs, rep)),
            dma((rep,)),
            dma((rep,)),
            dma((fs,)),
            dma((fs,)),
            dma((rep,)),
            dma((rep,)),
            dma((2, fs)),
            dma((2, fs)),
            dma((2, fs)),
            dma((fs,)),
            dma((fs,)),
            dma((3,)),
            dma((3,)),
            dma((10,)),
        ],
        compiler_params=pltpu.CompilerParams(
            collective_id=0, has_side_effects=True, vmem_limit_bytes=32 * 1024 * 1024
        ),
    )(
        *(
            pltpu.with_memory_space_constraint(operand, pltpu.HBM)
            for operand in (
                inputs,
                cot_query,
                cot_key,
                basis_query,
                basis_key,
                weight_query,
                weight_key,
                moments_query,
                moments_key,
            )
        )
    )

    steps = min(8, height // 16)
    tall, short = height * fs // steps, height // steps

    def fixed(*dims):
        return pl.BlockSpec(dims, lambda i: (0,) * len(dims))

    def banded(*dims):
        return pl.BlockSpec(dims, lambda i: (i, 0))

    owned = tuple(
        shape((height, columns), f32) for columns in (query_cols, key_cols, query_cols, key_cols)
    )
    owned_specs = tuple(
        banded(short, columns) for columns in (query_cols, key_cols, query_cols, key_cols)
    )
    return pl.pallas_call(
        functools.partial(
            apply, float(rank * query_cols * tp), float(rank * key_cols * tp)
        ),
        grid=(steps,),
        out_shape=owned
        + (
            shape((height * fs, query_cols), bf16),
            shape((height * fs, key_cols), bf16),
            shape((2, rows, query_cols), f32),
            shape((2, rows, key_cols), f32),
        ),
        in_specs=[
            fixed(2, 8, LANES),
            fixed(rank, query_cols),
            fixed(rank, key_cols),
            fixed(rows, query_cols),
            fixed(rows, key_cols),
            fixed(2, rows, query_cols),
            fixed(2, rows, key_cols),
            pl.BlockSpec((2, tall, rank), lambda i: (0, i, 0)),
            banded(tall, query_cols),
            banded(tall, key_cols),
            banded(short, rank),
            banded(short, rank),
            banded(short, query_cols),
            banded(short, key_cols),
        ],
        out_specs=owned_specs
        + (
            banded(tall, query_cols),
            banded(tall, key_cols),
            fixed(2, rows, query_cols),
            fixed(2, rows, key_cols),
        ),
        compiler_params=pltpu.CompilerParams(
            dimension_semantics=("arbitrary",), vmem_limit_bytes=32 * 1024 * 1024
        ),
    )(
        totals,
        dir_query,
        dir_key,
        low_query,
        low_key,
        moments_query,
        moments_key,
        basis_all,
        weight_query_all,
        weight_key_all,
        basis_query,
        basis_key,
        weight_query,
        weight_key,
    )


def solution(mesh):
    in_specs = (
        P(("fs", "rep"), None),
        P(("fs", "rep"), "tp"),
        P(("fs", "rep"), "tp"),
        P("fs", None),
        P("fs", None),
        P("fs", "tp"),
        P("fs", "tp"),
        P(None, "fs", "tp"),
        P(None, "fs", "tp"),
    )
    out_specs = (
        P("fs", "tp"),
        P("fs", "tp"),
        P("fs", "tp"),
        P("fs", "tp"),
        P(None, "tp"),
        P(None, "tp"),
        P(None, "fs", "tp"),
        P(None, "fs", "tp"),
    )
    return jax.shard_map(
        on_device, mesh=mesh, in_specs=in_specs, out_specs=out_specs, check_vma=False
    )
```
